32 devices in a mesh: fs: 16 (over z, y, x), tp: 2 (over core).
Axes of the slice: x: 2, y: 2, z: 4, core: 2. Of those that a mesh axis runs over, the one named last changes fastest.
Arguments:
- gate_pre: bfloat16 [8192, 3072], P('fs', 'tp'), may hold values from -6 to 6
- up_pre: bfloat16 [8192, 3072], P('fs', 'tp'), may hold values from -6 to 6
- cotangent: bfloat16 [8192, 2048], P('fs'), may hold values from -8 to 8
- gate_weight: bfloat16 [2048, 3072], P('fs', 'tp'), may hold values from -0.125 to 0.125
- up_weight: bfloat16 [2048, 3072], P('fs', 'tp'), may hold values from -0.125 to 0.125
- down_weight: bfloat16 [2048, 3072], P('fs', 'tp'), may hold values from -0.109375 to 0.109375
Outputs:
- grad_input: bfloat16 [8192, 2048], P('fs')
- grad_down: float32 [2048, 3072], P('fs', 'tp')
The draws below stay inside these ranges and needn't reach their ends.
All inputs are finite; a program needn't handle non-finite values.
Results may differ from the reference program's by a relative error of at most 0.014.
Values may be sent and summed in bfloat16 or wider, within the bound.
A program may use at most 128 MiB of HBM per device.

```python
import jax
import jax.numpy as jnp
from jax import lax

D = 2048
FF = 3072
TOKENS = 8192
N_TP = 2


def strengthened(result, stream_key, source, target, blocks, factor):
    def block_of(position):
        return (jnp.arange(result.shape[position]) // (result.shape[position] // blocks)).reshape((-1,) + (1,) * (result.ndim - 1 - position))

    one_side = jax.random.permutation(stream_key, blocks)[block_of(target)]
    far = (block_of(target) + blocks // 2) % blocks
    return jnp.where((block_of(source) == one_side) | (block_of(source) == far), factor * result, result)


def steps_of(stream_key, shape, pieces, smallest, top_value):
    factor_of, own = 1.0, jax.random.fold_in(stream_key, 6)
    for position, shards_of in pieces:
        heights = jnp.exp(jax.random.uniform(jax.random.fold_in(own, position), (shards_of,), jnp.float32, smallest / len(pieces), top_value / len(pieces)))
        factor_of = factor_of * jnp.repeat(heights, shape[position] // shards_of).reshape([-1 if axis == position else 1 for axis in range(len(shape))])
    return factor_of


def noise(rng, extent, scale, most, split=(), held_as=jnp.bfloat16):
    drawn = scale * jax.random.normal(rng, extent, jnp.float32)
    if split:
        drawn = drawn * steps_of(rng, extent, split, -0.22, 0.18)
    return jnp.clip(drawn, -most, most).astype(held_as)


def gaussian_with(rng, shape, scale, bound, pieces, heavy, dtype=jnp.bfloat16):
    drawn = scale * jax.random.normal(rng, shape, jnp.float32)
    if pieces:
        drawn = drawn * steps_of(rng, shape, pieces, -0.22, 0.18)
    return jnp.clip(strengthened(drawn, jax.random.fold_in(rng, 3), *heavy), -bound, bound).astype(dtype)


def setup_inputs(seed: int = 0) -> dict:
    arg_keys = jax.random.split(jax.random.key(seed), 7)
    gate_pre = noise(arg_keys[0], (TOKENS, FF), 1.0, 6.0, ((0, 16), (1, 2)))
    up_pre = noise(arg_keys[1], (TOKENS, FF), 1.0, 6.0, ((0, 16), (1, 2)))
    cotangent = gaussian_with(arg_keys[2], (TOKENS, D), 1.0, 8.0, ((0, 16),), (0, 1, 16, 2.0))
    gate_weight = noise(arg_keys[3], (D, FF), D ** -0.5, 0.125, ((0, 16), (1, 2)))
    up_weight = noise(arg_keys[4], (D, FF), D ** -0.5, 0.125, ((0, 16), (1, 2)))
    down_weight = noise(arg_keys[5], (D, FF), FF ** -0.5, 0.109375, ((0, 16), (1, 2)))
    return dict(gate_pre=gate_pre, up_pre=up_pre, cotangent=cotangent, gate_weight=gate_weight, up_weight=up_weight, down_weight=down_weight)


def reference(gate_pre, up_pre, cotangent, gate_weight, up_weight, down_weight):
    gate = gate_pre.astype(jnp.float32)
    upper = up_pre.astype(jnp.float32)
    sigma = jax.nn.sigmoid(gate)
    hidden = (gate * sigma * upper).astype(jnp.bfloat16)
    d_hidden = jnp.dot(cotangent, down_weight, preferred_element_type=jnp.float32)
    d_gate = (d_hidden * upper * sigma * (1.0 + gate * (1.0 - sigma))).astype(jnp.bfloat16)
    d_up = (d_hidden * gate * sigma).astype(jnp.bfloat16)
    grad_down = lax.dot_general(cotangent, hidden, (((0,), (0,)), ((), ())), preferred_element_type=jnp.float32)
    width = FF // N_TP
    total = jnp.zeros((cotangent.shape[0], D), jnp.float32)
    for block in range(N_TP):
        lower = block * width
        part = lax.dot_general(d_gate[:, lower:lower + width], gate_weight[:, lower:lower + width], (((1,), (1,)), ((), ())), preferred_element_type=jnp.float32)
        part = part + lax.dot_general(d_up[:, lower:lower + width], up_weight[:, lower:lower + width], (((1,), (1,)), ((), ())), preferred_element_type=jnp.float32)
        total = total + part.astype(jnp.bfloat16).astype(jnp.float32)
    return total.astype(jnp.bfloat16), grad_down
```

```python
import functools

import jax
import jax.numpy as jnp
from jax import lax
from jax.experimental import pallas as pl
from jax.experimental.pallas import tpu as pltpu
from jax.sharding import PartitionSpec as P

MESH = pl.DeviceIdType.MESH
F32, BF16 = jnp.float32, jnp.bfloat16
LANES = 128
VMEM_LIMIT = 60 * 1024 * 1024


def group_of(n_fs, width):
    for g in (4, 2):
        if n_fs % g == 0 and n_fs > g and width % (g * LANES) == 0:
            return g
    return 1


def place(g):
    fs, core = lax.axis_index("fs"), lax.axis_index("tp")
    base = lax.div(fs, g) * g
    return base, lax.rem(fs, g), core


def greet(g, base, me, core):
    barrier = pltpu.get_barrier_semaphore()
    for k in range(1, g):
        pl.semaphore_signal(barrier, inc=1, device_id=(base + lax.rem(me + k, g), core), device_id_type=MESH)
    pl.semaphore_signal(barrier, inc=1, device_id=(base + me, 1 - core), device_id_type=MESH)
    pl.semaphore_wait(barrier, g)


def remote(src, dst, send, recv, device):
    return pltpu.make_async_remote_copy(
        src_ref=src, dst_ref=dst, send_sem=send, recv_sem=recv, device_id=device, device_id_type=MESH
    )


def at(index, size):
    return pl.ds(pl.multiple_of(index * size, size), size)


def weights_kernel(g, *refs):
    ins, outs, (send, recv, own) = refs[:3], refs[3:6], refs[6:]
    base, me, core = place(g)
    greet(g, base, me, core)
    rows, part = ins[0].shape[0], ins[0].shape[1] // g
    copies = []
    for k in range(1, g):
        q = lax.rem(me + k, g)
        for i in (2, 0, 1):
            c = remote(ins[i].at[:, at(q, part)], outs[i].at[at(me, rows), :], send.at[i, k], recv.at[i, k], (base + q, core))
            c.start()
            copies.append(c)
    for i in range(3):
        c = pltpu.make_async_copy(ins[i].at[:, at(me, part)], outs[i].at[at(me, rows), :], own.at[i])
        c.start()
        copies.append(c)
    for c in copies:
        c.wait()


def tokens_kernel(g, gate, up, cot, gate_out, up_out, cot_out, send, recv, own):
    base, me, core = place(g)
    greet(g, base, me, core)
    rows, part = gate.shape[0], gate.shape[1] // g
    half = rows // 2
    firsts, others = [], []
    for k in range(1, g):
        q = lax.rem(me + k, g)
        c = remote(
            cot.at[at(core, half), :], cot_out.at[at(me * 2 + core, half), :], send.at[0, k], recv.at[0, k], (base + q, core)
        )
        c.start()
        firsts.append(c)
    for i, (a, b) in enumerate(((gate, gate_out), (up, up_out))):
        for k in range(1, g):
            q = lax.rem(me + k, g)
            c = remote(a.at[:, at(q, part)], b.at[at(me, rows), :], send.at[1 + i, k], recv.at[1 + i, k], (base + q, core))
            c.start()
            others.append(c)
        c = pltpu.make_async_copy(a.at[:, at(me, part)], b.at[at(me, rows), :], own.at[1 + i])
        c.start()
        others.append(c)
    c = pltpu.make_async_copy(cot, cot_out.at[at(me, rows), :], own.at[0])
    c.start()
    others.append(c)
    for k in range(1, g):
        firsts[k - 1].wait_recv()
        block = cot_out.at[at(lax.rem(me + g - k, g) * 2 + core, half), :]
        c = remote(block, block, send.at[3, k], recv.at[3, k], (base + me, 1 - core))
        c.start()
        others.append(c)
    for c in firsts:
        c.wait_send()
    for c in others:
        c.wait()


def outputs_kernel(g, part, down, out, down_out, sib, mine, got, down_got, send, recv):
    base, me, core = place(g)
    greet(g, base, me, core)
    rows, wide = out.shape
    half = wide // 2
    keep, give = at(core, half), at(1 - core, half)
    sibling = (base + me, 1 - core)
    drows, dwide = down_got.shape[1:]
    order = list(range(1, g)) + [0]
    crossed, downs, sums = {}, [], []
    for k in order:
        q = lax.rem(me + k, g)
        c = remote(part.at[at(q, rows), give], sib.at[k], send.at[0, k], recv.at[0, k], sibling)
        c.start()
        crossed[k] = c
    for k in range(1, g):
        q = lax.rem(me + k, g)
        c = remote(down.at[at(q, drows), :], down_got.at[k], send.at[1, k], recv.at[1, k], (base + q, core))
        c.start()
        downs.append(c)
    for k in order:
        q = lax.rem(me + k, g)
        crossed[k].wait_recv()
        total = part[at(q, rows), keep].astype(F32) + sib[k].astype(F32)
        mine[k] = total.astype(BF16)
        if k:
            c = remote(mine.at[k], got.at[k], send.at[2, k], recv.at[2, k], (base + q, core))
            c.start()
            sums.append(c)
    down_out[:, at(me, dwide)] = down[at(me, drows), :].astype(F32)
    for k in range(1, g):
        downs[k - 1].wait_recv()
        down_out[:, at(lax.rem(me + g - k, g), dwide)] = down_got[k].astype(F32)
    for c in sums:
        c.wait_recv()
    total = mine[0].astype(F32)
    for k in range(1, g):
        total = total + got[k].astype(F32)
    out[:, keep] = total.astype(BF16)
    last = remote(out.at[:, keep], out.at[:, keep], send.at[3, 0], recv.at[3, 0], sibling)
    last.start()
    for k in order:
        crossed[k].wait_send()
    for c in downs + sums:
        c.wait_send()
    last.wait()


def call(kernel, outs, scratch, ident, moved, *args):
    vmem = pl.BlockSpec(memory_space=pltpu.VMEM)
    return pl.pallas_call(
        kernel,
        out_shape=outs,
        in_specs=[vmem] * len(args),
        out_specs=[vmem] * len(outs),
        scratch_shapes=scratch,
        compiler_params=pltpu.CompilerParams(collective_id=ident, has_side_effects=True, vmem_limit_bytes=VMEM_LIMIT),
        cost_estimate=pl.CostEstimate(flops=0, bytes_accessed=moved * 40, transcendentals=0),
    )(*args)


def shared(g, n_fs, gate_pre, up_pre, cotangent, gate_weight, up_weight, down_weight):
    tokens, width = gate_pre.shape
    rows, depth = gate_weight.shape[0], cotangent.shape[1]
    part = width // g
    sems = pltpu.SemaphoreType.DMA
    struct = jax.ShapeDtypeStruct
    columns = [[o * g + p for o in range(n_fs // g)] for p in range(g)]
    block = struct((rows * g, part), BF16)
    blocks = call(
        functools.partial(weights_kernel, g), [block] * 3, [sems((3, g)), sems((3, g)), sems((3,))], 0,
        gate_weight.size * 6, gate_weight, up_weight, down_weight,
    )
    gather = functools.partial(lax.all_gather, axis_name="fs", axis_index_groups=columns, axis=0, tiled=True)
    down_all = gather(blocks[2])
    gate_w, up_w = gather(blocks[0]), gather(blocks[1])
    taken = struct((tokens * g, part), BF16)
    gates, ups, cots = call(
        functools.partial(tokens_kernel, g), [taken, taken, struct((tokens * g, depth), BF16)],
        [sems((4, g)), sems((4, g)), sems((3,))], 1, gate_pre.size * 8, gate_pre, up_pre, cotangent,
    )
    gate, upper = gates.astype(F32), ups.astype(F32)
    sigma = jax.nn.sigmoid(gate)
    hidden = (gate * sigma * upper).astype(BF16)
    share = lax.dot_general(cots, hidden, (((0,), (0,)), ((), ())), preferred_element_type=F32).astype(BF16)
    grad_down = lax.psum_scatter(share, "fs", scatter_dimension=0, axis_index_groups=columns, tiled=True)
    d_hidden = jnp.dot(cots, down_all, preferred_element_type=F32)
    d_gate = (d_hidden * upper * sigma * (1.0 + gate * (1.0 - sigma))).astype(BF16)
    d_up = (d_hidden * gate * sigma).astype(BF16)
    over = (((1,), (1,)), ((), ()))
    partial_sum = lax.dot_general(d_gate, gate_w, over, preferred_element_type=F32)
    partial_sum = partial_sum + lax.dot_general(d_up, up_w, over, preferred_element_type=F32)
    strip = (g, tokens, depth // 2)
    grad_input, grad_down = call(
        functools.partial(outputs_kernel, g),
        [struct((tokens, depth), BF16), struct((rows, width), F32)],
        [pltpu.VMEM(strip, BF16)] * 3 + [pltpu.VMEM((g, rows, part), BF16), sems((4, g)), sems((4, g))],
        2, cotangent.size * 8, partial_sum.astype(BF16), grad_down,
    )
    return grad_input, grad_down


def plain(gate_pre, up_pre, cotangent, gate_weight, up_weight, down_weight):
    gate = gate_pre.astype(F32)
    upper = up_pre.astype(F32)
    sigma = jax.nn.sigmoid(gate)
    hidden = (gate * sigma * upper).astype(BF16)
    share = lax.dot_general(cotangent, hidden, (((0,), (0,)), ((), ())), preferred_element_type=F32)
    grad_down = lax.psum_scatter(share, "fs", scatter_dimension=0, tiled=True)
    d_hidden = jnp.dot(cotangent, lax.all_gather(down_weight, "fs", axis=0, tiled=True), preferred_element_type=F32)
    d_gate = (d_hidden * upper * sigma * (1.0 + gate * (1.0 - sigma))).astype(BF16)
    d_up = (d_hidden * gate * sigma).astype(BF16)
    gate_w, up_w = lax.all_gather((gate_weight, up_weight), "fs", axis=0, tiled=True)
    over = (((1,), (1,)), ((), ()))
    partial_sum = lax.dot_general(d_gate, gate_w, over, preferred_element_type=F32)
    partial_sum = partial_sum + lax.dot_general(d_up, up_w, over, preferred_element_type=F32)
    grad_input = lax.psum(partial_sum.astype(BF16), "tp").astype(F32).astype(BF16)
    return grad_input, grad_down


def solution(mesh):
    n_fs, n_tp = mesh.shape["fs"], mesh.shape["tp"]

    def local(*args):
        g = group_of(n_fs, args[0].shape[1]) if n_tp == 2 else 1
        return shared(g, n_fs, *args) if g > 1 else plain(*args)

    both, rows = P("fs", "tp"), P("fs", None)
    return jax.shard_map(
        local, mesh=mesh, in_specs=(both, both, rows, both, both, both), out_specs=(rows, both), check_vma=False
    )
```

```python
import functools

import jax
import jax.numpy as jnp
from jax import lax
from jax.experimental import pallas as pl
from jax.experimental.pallas import tpu as pltpu
from jax.sharding import PartitionSpec as P

MESH = pl.DeviceIdType.MESH
F32, BF16 = jnp.float32, jnp.bfloat16
LANES = 128
VMEM_LIMIT = 60 * 1024 * 1024


def group_of(n_fs, width):
    return 4 if n_fs % 4 == 0 and n_fs > 4 and width % (4 * LANES) == 0 else 1


def place(g):
    fs, core = lax.axis_index("fs"), lax.axis_index("tp")
    return lax.div(fs, g) * g, lax.rem(fs, g), core


def greet(devices):
    barrier = pltpu.get_barrier_semaphore()
    for device in devices:
        pl.semaphore_signal(barrier, inc=1, device_id=device, device_id_type=MESH)
    pl.semaphore_wait(barrier, len(devices))


def remote(src, dst, send, recv, device):
    return pltpu.make_async_remote_copy(
        src_ref=src, dst_ref=dst, send_sem=send, recv_sem=recv, device_id=device, device_id_type=MESH
    )


def at(index, size):
    return pl.ds(pl.multiple_of(index * size, size), size)


def peers(g, base, me, core):
    return [(base + lax.rem(me + k, g), core) for k in range(1, g)]


def square(base, me, core):
    x, y = lax.rem(me, 2), lax.div(me, 2)
    xn, yn = y * 2 + (1 - x), (1 - y) * 2 + x
    return xn, yn, 3 - me, (base + xn, core), (base + yn, core), (base + me, 1 - core)


def swap_kernel(g, n, *refs):
    ins, outs, (send, recv, own) = refs[:n], refs[n : 2 * n], refs[2 * n :]
    base, me, core = place(g)
    greet(peers(g, base, me, core))
    rows, part = ins[0].shape[0], ins[0].shape[1] // g
    copies = []
    for k in range(1, g):
        q = lax.rem(me + k, g)
        for i in range(n):
            c = remote(ins[i].at[:, at(q, part)], outs[i].at[at(me, rows), :], send.at[i, k], recv.at[i, k], (base + q, core))
            c.start()
            copies.append(c)
    for i in range(n):
        c = pltpu.make_async_copy(ins[i].at[:, at(me, part)], outs[i].at[at(me, rows), :], own.at[i])
        c.start()
        copies.append(c)
    for c in copies:
        c.wait()


def tokens_kernel(g, n_out, cot, block, cot_out, gathered, send, recv, zsend, zrecv, own):
    base, me, core = place(g)
    outer = lax.div(base, g)
    xn, yn, far, xdev, ydev, sibling = square(base, me, core)
    others = [(lax.rem(outer + j, n_out) * g + me, core) for j in range(1, n_out)]
    greet([xdev, ydev, sibling] + others)
    half, wide = cot.shape[0] // 2, cot.shape[1] // 2
    cols = [pl.ds(0, wide), pl.ds(wide, wide)]
    mine = at(core, half)
    piece = lambda owner, i: cot_out.at[at(owner * 2 + core, half), cols[i]]
    started, passed = [], []

    def go(n, a, b, device):
        c = remote(a, b, send.at[n], recv.at[n], device)
        c.start()
        started.append(c)
        return c

    def pass_on(n, owner, i):
        c = remote(piece(owner, i), piece(owner, i), send.at[n], recv.at[n], sibling)
        c.start()
        passed.append(c)

    x0 = go(0, cot.at[mine, cols[0]], piece(me, 0), xdev)
    y1 = go(1, cot.at[mine, cols[1]], piece(me, 1), ydev)
    x1 = go(2, cot.at[mine, cols[1]], piece(me, 1), xdev)
    y0 = go(3, cot.at[mine, cols[0]], piece(me, 0), ydev)
    rows = block.shape[0]
    for j in range(1, n_out):
        c = remote(block, gathered.at[at(outer, rows), :], zsend.at[j], zrecv.at[j], others[j - 1])
        c.start()
        passed.append(c)
    for i, (a, b) in enumerate(((cot, cot_out.at[at(me, 2 * half), :]), (block, gathered.at[at(outer, rows), :]))):
        c = pltpu.make_async_copy(a, b, own.at[i])
        c.start()
        passed.append(c)
    x0.wait_recv()
    fy = go(4, piece(xn, 0), piece(xn, 0), ydev)
    pass_on(6, xn, 0)
    y1.wait_recv()
    fx = go(5, piece(yn, 1), piece(yn, 1), xdev)
    pass_on(7, yn, 1)
    x1.wait_recv()
    pass_on(8, xn, 1)
    y0.wait_recv()
    pass_on(9, yn, 0)
    fy.wait_recv()
    pass_on(10, far, 0)
    fx.wait_recv()
    pass_on(11, far, 1)
    for c in started:
        c.wait_send()
    for c in passed:
        c.wait()


def middle_kernel(g, gate, up, cots, down, hidden, d_gate, d_up, gates, ups, dh, send, recv, own):
    base, me, core = place(g)
    greet(peers(g, base, me, core))
    rows, part = gate.shape[0], gate.shape[1] // g
    copies = {}
    for k in range(1, g):
        q = lax.rem(me + k, g)
        for i, (a, b) in enumerate(((gate, gates), (up, ups))):
            c = remote(a.at[:, at(q, part)], b.at[at(me, rows), :], send.at[i, k], recv.at[i, k], (base + q, core))
            c.start()
            copies[i, k] = c
    for i, (a, b) in enumerate(((gate, gates), (up, ups))):
        c = pltpu.make_async_copy(a.at[:, at(me, part)], b.at[at(me, rows), :], own.at[i])
        c.start()
        copies[i, 0] = c
    tile = rows // 2

    def multiply(i, carry):
        dh[at(i, tile), :] = jnp.dot(cots[at(i, tile), :], down[...], preferred_element_type=F32)
        return carry

    lax.fori_loop(0, 2 * g, multiply, 0)
    strip = rows // 16
    for k in range(g):
        for i in range(2):
            if k:
                copies[i, k].wait_recv()
            else:
                copies[i, k].wait()
        owner = lax.rem(me + g - k, g)

        def pointwise(i, carry):
            r = at(owner * 16 + i, strip)
            gv, uv, dv = gates[r, :].astype(F32), ups[r, :].astype(F32), dh[r, :]
            s = jax.nn.sigmoid(gv)
            gs = gv * s
            hidden[r, :] = (gs * uv).astype(BF16)
            d_gate[r, :] = (dv * uv * s * (1.0 + gv * (1.0 - s))).astype(BF16)
            d_up[r, :] = (dv * gs).astype(BF16)
            return carry

        lax.fori_loop(0, 16, pointwise, 0)
    for k in range(1, g):
        for i in range(2):
            copies[i, k].wait_send()


OVER = (((1,), (1,)), ((), ()))


def input_kernel(g, d_gate, d_up, gate_w, up_w, out, give_buf, sib, mine, got, halves, send, recv):
    base, me, core = place(g)
    xn, yn, far, xdev, ydev, sibling = square(base, me, core)
    greet([xdev, ydev, sibling])
    rows, wide = out.shape[0], out.shape[1] // 2
    keep = at(core, wide)
    tile = rows // 2
    top, low = pl.ds(0, tile), pl.ds(tile, tile)
    sends, waits = [], []

    def product(side, owner, dst):
        cols = at(side, wide)

        def step(i, carry):
            r = at(owner * 2 + i, tile)
            total = lax.dot_general(d_gate[r, :], gate_w[cols, :], OVER, preferred_element_type=F32)
            total = total + lax.dot_general(d_up[r, :], up_w[cols, :], OVER, preferred_element_type=F32)
            dst[at(i, tile), :] = total.astype(BF16)
            return carry

        lax.fori_loop(0, 2, step, 0)

    def add(dst, where, src):
        dst[where, :] = (dst[where, :].astype(F32) + src[...].astype(F32)).astype(BF16)

    def go(n, a, b, device):
        c = remote(a, b, send.at[n], recv.at[n], device)
        c.start()
        sends.append(c)
        return c

    def chunk(k, owner):
        product(1 - core, owner, give_buf.at[k])
        c = go(k, give_buf.at[k], sib.at[k], sibling)
        product(core, owner, mine.at[k])
        c.wait_recv()
        add(mine.at[k], pl.ds(0, rows), sib.at[k])

    chunk(0, far)
    hx = go(4, mine.at[0, top, :], halves.at[0], xdev)
    hy = go(5, mine.at[0, low, :], halves.at[1], ydev)
    chunk(1, xn)
    waits.append(go(6, mine.at[1, top, :], got.at[0, top, :], xdev))
    chunk(2, yn)
    waits.append(go(7, mine.at[2, low, :], got.at[1, low, :], ydev))
    hy.wait_recv()
    add(mine.at[1], low, halves.at[1])
    waits.append(go(8, mine.at[1, low, :], got.at[0, low, :], xdev))
    hx.wait_recv()
    add(mine.at[2], top, halves.at[0])
    waits.append(go(9, mine.at[2, top, :], got.at[1, top, :], ydev))
    chunk(3, me)
    lasts = []
    for n, where, ready in ((10, top, (0, 3)), (11, low, (1, 2))):
        for i in ready:
            waits[i].wait_recv()
        total = mine[3, where, :].astype(F32) + got[0, where, :].astype(F32) + got[1, where, :].astype(F32)
        out[where, keep] = total.astype(BF16)
        lasts.append(go(n, out.at[where, keep], out.at[where, keep], sibling))
    for c in lasts:
        c.wait_recv()
    for c in sends:
        c.wait_send()


def down_kernel(g, down, out, got, send, recv):
    base, me, core = place(g)
    greet(peers(g, base, me, core))
    rows, wide = got.shape[1:]
    copies = []
    for k in range(1, g):
        q = lax.rem(me + k, g)
        c = remote(down.at[at(q, rows), :], got.at[k], send.at[k], recv.at[k], (base + q, core))
        c.start()
        copies.append(c)
    out[:, at(me, wide)] = down[at(me, rows), :].astype(F32)
    for k in range(1, g):
        copies[k - 1].wait_recv()
        out[:, at(lax.rem(me + g - k, g), wide)] = got[k].astype(F32)
    for c in copies:
        c.wait_send()


def call(kernel, outs, scratch, ident, cost, *args):
    vmem = pl.BlockSpec(memory_space=pltpu.VMEM)
    return pl.pallas_call(
        kernel,
        out_shape=outs,
        in_specs=[vmem] * len(args),
        out_specs=[vmem] * len(outs),
        scratch_shapes=scratch,
        compiler_params=pltpu.CompilerParams(collective_id=ident, has_side_effects=True, vmem_limit_bytes=VMEM_LIMIT),
        cost_estimate=pl.CostEstimate(flops=0, bytes_accessed=cost, transcendentals=0),
    )(*args)


def shared(g, n_fs, gate_pre, up_pre, cotangent, gate_weight, up_weight, down_weight):
    tokens, width = gate_pre.shape
    rows, depth = gate_weight.shape[0], cotangent.shape[1]
    part, n_out, all_tokens = width // g, n_fs // g, tokens * g
    sems, vmem = pltpu.SemaphoreType.DMA, pltpu.VMEM
    struct = jax.ShapeDtypeStruct
    us = 3_000_000
    columns = [[o * g + p for o in range(n_out)] for p in range(g)]
    gather = functools.partial(lax.all_gather, axis_name="fs", axis_index_groups=columns, axis=0, tiled=True)

    def swap(ident, *weights):
        n = len(weights)
        return call(
            functools.partial(swap_kernel, g, n), [struct((rows * g, part), BF16)] * n,
            [sems((n, g)), sems((n, g)), sems((n,))], ident, 7 * n * us, *weights,
        )

    down_all = gather(swap(0, down_weight)[0])
    gate_block, up_block = swap(1, gate_weight, up_weight)
    up_w = gather(up_block)
    cots, gate_w = call(
        functools.partial(tokens_kernel, g, n_out), [struct((all_tokens, depth), BF16), struct((depth, part), BF16)],
        [sems((12,)), sems((12,)), sems((n_out,)), sems((n_out,)), sems((2,))], 2, 40 * us, cotangent, gate_block,
    )
    wide = struct((all_tokens, part), BF16)
    hidden, d_gate, d_up = call(
        functools.partial(middle_kernel, g), [wide] * 3,
        [vmem(wide.shape, BF16)] * 2 + [vmem(wide.shape, F32), sems((2, g)), sems((2, g)), sems((2,))],
        3, 40 * us, gate_pre, up_pre, cots, down_all,
    )
    share = lax.dot_general(cots, hidden, (((0,), (0,)), ((), ())), preferred_element_type=F32).astype(BF16)
    grad_block = lax.psum_scatter(share, "fs", scatter_dimension=0, axis_index_groups=columns, tiled=True)
    side = depth // 2
    grad_input = call(
        functools.partial(input_kernel, g), [struct((tokens, depth), BF16)],
        [vmem((4, tokens, side), BF16)] * 3 + [vmem((2, tokens, side), BF16), vmem((2, tokens // 2, side), BF16)]
        + [sems((12,)), sems((12,))],
        4, 50 * us, d_gate, d_up, gate_w, up_w,
    )[0]
    grad_down = call(
        functools.partial(down_kernel, g), [struct((rows, width), F32)],
        [vmem((g, rows, part), BF16), sems((g,)), sems((g,))], 5, 6 * us, grad_block,
    )[0]
    return grad_input, grad_down


def plain(gate_pre, up_pre, cotangent, gate_weight, up_weight, down_weight):
    gate = gate_pre.astype(F32)
    upper = up_pre.astype(F32)
    sigma = jax.nn.sigmoid(gate)
    hidden = (gate * sigma * upper).astype(BF16)
    share = lax.dot_general(cotangent, hidden, (((0,), (0,)), ((), ())), preferred_element_type=F32)
    grad_down = lax.psum_scatter(share, "fs", scatter_dimension=0, tiled=True)
    d_hidden = jnp.dot(cotangent, lax.all_gather(down_weight, "fs", axis=0, tiled=True), preferred_element_type=F32)
    d_gate = (d_hidden * upper * sigma * (1.0 + gate * (1.0 - sigma))).astype(BF16)
    d_up = (d_hidden * gate * sigma).astype(BF16)
    gate_w, up_w = lax.all_gather((gate_weight, up_weight), "fs", axis=0, tiled=True)
    over = (((1,), (1,)), ((), ()))
    partial_sum = lax.dot_general(d_gate, gate_w, over, preferred_element_type=F32)
    partial_sum = partial_sum + lax.dot_general(d_up, up_w, over, preferred_element_type=F32)
    grad_input = lax.psum(partial_sum.astype(BF16), "tp").astype(F32).astype(BF16)
    return grad_input, grad_down


def solution(mesh):
    n_fs, n_tp = mesh.shape["fs"], mesh.shape["tp"]

    def local(*args):
        g = group_of(n_fs, args[0].shape[1]) if n_tp == 2 else 1
        return shared(g, n_fs, *args) if g > 1 else plain(*args)

    both, rows = P("fs", "tp"), P("fs", None)
    return jax.shard_map(
        local, mesh=mesh, in_specs=(both, both, rows, both, both, both), out_specs=(rows, both), check_vma=False
    )
```

```python
import functools

import jax
import jax.numpy as jnp
from jax import lax
from jax.experimental import pallas as pl
from jax.experimental.pallas import tpu as pltpu
from jax.sharding import PartitionSpec as P

MESH = pl.DeviceIdType.MESH
F32, BF16 = jnp.float32, jnp.bfloat16
LANES = 128
VMEM_LIMIT = 60 * 1024 * 1024


def group_of(n_fs, width):
    return 4 if n_fs % 4 == 0 and n_fs > 4 and width % (4 * LANES) == 0 else 1


def place(g):
    fs, core = lax.axis_index("fs"), lax.axis_index("tp")
    return lax.div(fs, g) * g, lax.rem(fs, g), core


def greet(devices):
    barrier = pltpu.get_barrier_semaphore()
    for device in devices:
        pl.semaphore_signal(barrier, inc=1, device_id=device, device_id_type=MESH)
    pl.semaphore_wait(barrier, len(devices))


def remote(src, dst, send, recv, device):
    return pltpu.make_async_remote_copy(
        src_ref=src, dst_ref=dst, send_sem=send, recv_sem=recv, device_id=device, device_id_type=MESH
    )


def at(index, size):
    return pl.ds(pl.multiple_of(index * size, size), size)


def peers(g, base, me, core):
    return [(base + lax.rem(me + k, g), core) for k in range(1, g)]


def square(base, me, core):
    x, y = lax.rem(me, 2), lax.div(me, 2)
    xn, yn = y * 2 + (1 - x), (1 - y) * 2 + x
    return xn, yn, 3 - me, (base + xn, core), (base + yn, core), (base + me, 1 - core)


class Ring:
    def __init__(self, array, rows, outer, n_out, base, me, core, g, send, recv, line):
        self.array, self.half, self.outer, self.n = array, rows // 2, outer, n_out
        self.send, self.recv, self.line, self.copies = send, recv, line, []
        self.devices = [(lax.rem(outer + d, n_out) * g + me, core) for d in (1, n_out - 1)]

    def step(self, s):
        if s:
            for c in self.copies[-2:]:
                c.wait_recv()
        if s == self.n - 1:
            return
        for way in range(2):
            owner = lax.rem(self.outer + (self.n - s if way == 0 else s), self.n)
            block = self.array.at[at(owner * 2 + way, self.half), :]
            n = s * 2 + way
            c = remote(block, block, self.send.at[self.line, n], self.recv.at[self.line, n], self.devices[way])
            c.start()
            self.copies.append(c)

    def finish(self):
        for c in self.copies:
            c.wait_send()


def ring_devices(outer, n_out, me, core, g):
    return [(lax.rem(outer + d, n_out) * g + me, core) for d in (1, n_out - 1)]


def tokens_kernel(g, n_out, cot, down, gate, up, cot_out, down_all, gate_all, up_block, send, recv, wsend, wrecv, zsend, zrecv, own):
    base, me, core = place(g)
    outer = lax.div(base, g)
    xn, yn, far, xdev, ydev, sibling = square(base, me, core)
    greet(peers(g, base, me, core) + [sibling] + ring_devices(outer, n_out, me, core, g))
    half, wide = cot.shape[0] // 2, cot.shape[1] // 2
    rows, part = down.shape[0], down.shape[1] // g
    cols = [pl.ds(0, wide), pl.ds(wide, wide)]
    mine = at(core, half)
    piece = lambda owner, i: cot_out.at[at(owner * 2 + core, half), cols[i]]
    started, passed, swaps = [], [], {}

    def go(n, a, b, device):
        c = remote(a, b, send.at[n], recv.at[n], device)
        c.start()
        started.append(c)
        return c

    def pass_on(n, owner, i):
        c = remote(piece(owner, i), piece(owner, i), send.at[n], recv.at[n], sibling)
        c.start()
        passed.append(c)

    def local_copy(i, a, b):
        c = pltpu.make_async_copy(a, b, own.at[i])
        c.start()
        return c

    def swap(i, a, b):
        swaps[i] = []
        for k in range(1, g):
            q = lax.rem(me + k, g)
            c = remote(a.at[:, at(q, part)], b, wsend.at[i, k], wrecv.at[i, k], (base + q, core))
            c.start()
            swaps[i].append(c)
        return local_copy(i, a.at[:, at(me, part)], b)

    place_of = at(outer * g + me, rows)
    own_down = swap(0, down, down_all.at[place_of, :])
    own_gate = swap(1, gate, gate_all.at[place_of, :])
    x0 = go(0, cot.at[mine, cols[0]], piece(me, 0), xdev)
    y1 = go(1, cot.at[mine, cols[1]], piece(me, 1), ydev)
    x1 = go(2, cot.at[mine, cols[1]], piece(me, 1), xdev)
    y0 = go(3, cot.at[mine, cols[0]], piece(me, 0), ydev)
    own_cot = local_copy(3, cot, cot_out.at[at(me, 2 * half), :])
    rings = []
    for i, array, mine_copy in ((0, down_all, own_down), (1, gate_all, own_gate)):
        mine_copy.wait()
        for c in swaps[i]:
            c.wait_recv()
        rings.append(Ring(array, rows * g, outer, n_out, base, me, core, g, zsend, zrecv, i))
        rings[i].step(0)
    steps = [(i, n) for n in range(1, n_out) for i in range(2)]

    def turn():
        if steps:
            i, n = steps.pop(0)
            rings[i].step(n)

    turn()
    x0.wait_recv()
    fy = go(4, piece(xn, 0), piece(xn, 0), ydev)
    pass_on(6, xn, 0)
    y1.wait_recv()
    fx = go(5, piece(yn, 1), piece(yn, 1), xdev)
    pass_on(7, yn, 1)
    own_up = swap(2, up, up_block.at[at(me, rows), :])
    turn()
    turn()
    x1.wait_recv()
    pass_on(8, xn, 1)
    y0.wait_recv()
    pass_on(9, yn, 0)
    turn()
    fy.wait_recv()
    pass_on(10, far, 0)
    fx.wait_recv()
    pass_on(11, far, 1)
    while steps:
        turn()
    own_cot.wait()
    own_up.wait()
    for c in swaps[2]:
        c.wait_recv()
    for c in started + swaps[0] + swaps[1] + swaps[2]:
        c.wait_send()
    for c in passed:
        c.wait()
    for r in rings:
        r.finish()


def middle_kernel(g, n_out, gate, up, cots, down, block, hidden, d_gate, d_up, up_all, gates, ups, dh, send, recv, zsend, zrecv, own):
    base, me, core = place(g)
    outer = lax.div(base, g)
    greet(peers(g, base, me, core) + ring_devices(outer, n_out, me, core, g))
    first = pltpu.make_async_copy(block, up_all.at[at(outer, block.shape[0]), :], own.at[2])
    first.start()
    rows, part = gate.shape[0], gate.shape[1] // g
    copies = {}
    for k in range(1, g):
        q = lax.rem(me + k, g)
        for i, (a, b) in enumerate(((gate, gates), (up, ups))):
            c = remote(a.at[:, at(q, part)], b.at[at(me, rows), :], send.at[i, k], recv.at[i, k], (base + q, core))
            c.start()
            copies[i, k] = c
    for i, (a, b) in enumerate(((gate, gates), (up, ups))):
        c = pltpu.make_async_copy(a.at[:, at(me, part)], b.at[at(me, rows), :], own.at[i])
        c.start()
        copies[i, 0] = c
    first.wait()
    ring = Ring(up_all, block.shape[0], outer, n_out, base, me, core, g, zsend, zrecv, 0)
    ring.step(0)
    tile = rows // 2

    def multiply(i, carry):
        dh[at(i, tile), :] = jnp.dot(cots[at(i, tile), :], down[...], preferred_element_type=F32)
        return carry

    lax.fori_loop(0, 2 * g, multiply, 0)
    steps = list(range(1, n_out))
    strip = rows // 16
    for k in range(g):
        if steps:
            ring.step(steps.pop(0))
        for i in range(2):
            if k:
                copies[i, k].wait_recv()
            else:
                copies[i, k].wait()
        owner = lax.rem(me + g - k, g)

        def pointwise(i, carry):
            r = at(owner * 16 + i, strip)
            gv, uv, dv = gates[r, :].astype(F32), ups[r, :].astype(F32), dh[r, :]
            s = jax.nn.sigmoid(gv)
            gs = gv * s
            hidden[r, :] = (gs * uv).astype(BF16)
            d_gate[r, :] = (dv * uv * s * (1.0 + gv * (1.0 - s))).astype(BF16)
            d_up[r, :] = (dv * gs).astype(BF16)
            return carry

        lax.fori_loop(0, 16, pointwise, 0)
    while steps:
        ring.step(steps.pop(0))
    ring.finish()
    for k in range(1, g):
        for i in range(2):
            copies[i, k].wait_send()


OVER = (((1,), (1,)), ((), ()))


def input_kernel(g, d_gate, d_up, gate_w, up_w, out, give_buf, sib, mine, got, halves, send, recv):
    base, me, core = place(g)
    xn, yn, far, xdev, ydev, sibling = square(base, me, core)
    greet([xdev, ydev, sibling])
    rows, wide = out.shape[0], out.shape[1] // 2
    keep = at(core, wide)
    tile = rows // 2
    top, low = pl.ds(0, tile), pl.ds(tile, tile)
    sends, waits = [], []

    def product(side, owner, dst):
        cols = at(side, wide)

        def step(i, carry):
            r = at(owner * 2 + i, tile)
            total = lax.dot_general(d_gate[r, :], gate_w[cols, :], OVER, preferred_element_type=F32)
            total = total + lax.dot_general(d_up[r, :], up_w[cols, :], OVER, preferred_element_type=F32)
            dst[at(i, tile), :] = total.astype(BF16)
            return carry

        lax.fori_loop(0, 2, step, 0)

    def add(dst, where, src):
        dst[where, :] = (dst[where, :].astype(F32) + src[...].astype(F32)).astype(BF16)

    def go(n, a, b, device):
        c = remote(a, b, send.at[n], recv.at[n], device)
        c.start()
        sends.append(c)
        return c

    def chunk(k, owner):
        product(1 - core, owner, give_buf.at[k])
        c = go(k, give_buf.at[k], sib.at[k], sibling)
        product(core, owner, mine.at[k])
        c.wait_recv()
        add(mine.at[k], pl.ds(0, rows), sib.at[k])

    chunk(0, far)
    hx = go(4, mine.at[0, top, :], halves.at[0], xdev)
    hy = go(5, mine.at[0, low, :], halves.at[1], ydev)
    chunk(1, xn)
    waits.append(go(6, mine.at[1, top, :], got.at[0, top, :], xdev))
    chunk(2, yn)
    waits.append(go(7, mine.at[2, low, :], got.at[1, low, :], ydev))
    hy.wait_recv()
    add(mine.at[1], low, halves.at[1])
    waits.append(go(8, mine.at[1, low, :], got.at[0, low, :], xdev))
    hx.wait_recv()
    add(mine.at[2], top, halves.at[0])
    waits.append(go(9, mine.at[2, top, :], got.at[1, top, :], ydev))
    chunk(3, me)
    lasts = []
    for n, where, ready in ((10, top, (0, 3)), (11, low, (1, 2))):
        for i in ready:
            waits[i].wait_recv()
        total = mine[3, where, :].astype(F32) + got[0, where, :].astype(F32) + got[1, where, :].astype(F32)
        out[where, keep] = total.astype(BF16)
        lasts.append(go(n, out.at[where, keep], out.at[where, keep], sibling))
    for c in lasts:
        c.wait_recv()
    for c in sends:
        c.wait_send()


def down_kernel(g, down, out, got, send, recv):
    base, me, core = place(g)
    greet(peers(g, base, me, core))
    rows, wide = got.shape[1:]
    copies = []
    for k in range(1, g):
        q = lax.rem(me + k, g)
        c = remote(down.at[at(q, rows), :], got.at[k], send.at[k], recv.at[k], (base + q, core))
        c.start()
        copies.append(c)
    out[:, at(me, wide)] = down[at(me, rows), :].astype(F32)
    for k in range(1, g):
        copies[k - 1].wait_recv()
        out[:, at(lax.rem(me + g - k, g), wide)] = got[k].astype(F32)
    for c in copies:
        c.wait_send()


def call(kernel, outs, scratch, ident, cost, *args):
    vmem = pl.BlockSpec(memory_space=pltpu.VMEM)
    return pl.pallas_call(
        kernel,
        out_shape=outs,
        in_specs=[vmem] * len(args),
        out_specs=[vmem] * len(outs),
        scratch_shapes=scratch,
        compiler_params=pltpu.CompilerParams(collective_id=ident, has_side_effects=True, vmem_limit_bytes=VMEM_LIMIT),
        cost_estimate=pl.CostEstimate(flops=0, bytes_accessed=cost, transcendentals=0),
    )(*args)


def shared(g, n_fs, gate_pre, up_pre, cotangent, gate_weight, up_weight, down_weight):
    tokens, width = gate_pre.shape
    rows, depth = gate_weight.shape[0], cotangent.shape[1]
    part, n_out, all_tokens = width // g, n_fs // g, tokens * g
    sems, vmem = pltpu.SemaphoreType.DMA, pltpu.VMEM
    struct = jax.ShapeDtypeStruct
    us = 3_000_000
    columns = [[o * g + p for o in range(n_out)] for p in range(g)]
    every, block = struct((depth, part), BF16), struct((rows * g, part), BF16)
    cots, down_all, gate_w, up_block = call(
        functools.partial(tokens_kernel, g, n_out), [struct((all_tokens, depth), BF16), every, every, block],
        [sems((12,)), sems((12,)), sems((3, g)), sems((3, g)), sems((2, 2 * n_out)), sems((2, 2 * n_out)), sems((4,))],
        0, 60 * us, cotangent, down_weight, gate_weight, up_weight,
    )
    wide = struct((all_tokens, part), BF16)
    hidden, d_gate, d_up, up_w = call(
        functools.partial(middle_kernel, g, n_out), [wide] * 3 + [every],
        [vmem(wide.shape, BF16)] * 2
        + [vmem(wide.shape, F32), sems((2, g)), sems((2, g)), sems((1, 2 * n_out)), sems((1, 2 * n_out)), sems((3,))],
        1, 40 * us, gate_pre, up_pre, cots, down_all, up_block,
    )
    share = lax.dot_general(cots, hidden, (((0,), (0,)), ((), ())), preferred_element_type=F32).astype(BF16)
    grad_block = lax.psum_scatter(share, "fs", scatter_dimension=0, axis_index_groups=columns, tiled=True)
    side = depth // 2
    grad_input = call(
        functools.partial(input_kernel, g), [struct((tokens, depth), BF16)],
        [vmem((4, tokens, side), BF16)] * 3 + [vmem((2, tokens, side), BF16), vmem((2, tokens // 2, side), BF16)]
        + [sems((12,)), sems((12,))],
        2, 50 * us, d_gate, d_up, gate_w, up_w,
    )[0]
    grad_down = call(
        functools.partial(down_kernel, g), [struct((rows, width), F32)],
        [vmem((g, rows, part), BF16), sems((g,)), sems((g,))], 3, 6 * us, grad_block,
    )[0]
    return grad_input, grad_down


def plain(gate_pre, up_pre, cotangent, gate_weight, up_weight, down_weight):
    gate = gate_pre.astype(F32)
    upper = up_pre.astype(F32)
    sigma = jax.nn.sigmoid(gate)
    hidden = (gate * sigma * upper).astype(BF16)
    share = lax.dot_general(cotangent, hidden, (((0,), (0,)), ((), ())), preferred_element_type=F32)
    grad_down = lax.psum_scatter(share, "fs", scatter_dimension=0, tiled=True)
    d_hidden = jnp.dot(cotangent, lax.all_gather(down_weight, "fs", axis=0, tiled=True), preferred_element_type=F32)
    d_gate = (d_hidden * upper * sigma * (1.0 + gate * (1.0 - sigma))).astype(BF16)
    d_up = (d_hidden * gate * sigma).astype(BF16)
    gate_w, up_w = lax.all_gather((gate_weight, up_weight), "fs", axis=0, tiled=True)
    over = (((1,), (1,)), ((), ()))
    partial_sum = lax.dot_general(d_gate, gate_w, over, preferred_element_type=F32)
    partial_sum = partial_sum + lax.dot_general(d_up, up_w, over, preferred_element_type=F32)
    grad_input = lax.psum(partial_sum.astype(BF16), "tp").astype(F32).astype(BF16)
    return grad_input, grad_down


def solution(mesh):
    n_fs, n_tp = mesh.shape["fs"], mesh.shape["tp"]

    def local(*args):
        g = group_of(n_fs, args[0].shape[1]) if n_tp == 2 else 1
        return shared(g, n_fs, *args) if g > 1 else plain(*args)

    both, rows = P("fs", "tp"), P("fs", None)
    return jax.shard_map(
        local, mesh=mesh, in_specs=(both, both, rows, both, both, both), out_specs=(rows, both), check_vma=False
    )
```

```python
import functools

import jax
import jax.numpy as jnp
from jax import lax
from jax.experimental import pallas as pl
from jax.experimental.pallas import tpu as pltpu
from jax.sharding import PartitionSpec as P

MESH = pl.DeviceIdType.MESH
F32, BF16 = jnp.float32, jnp.bfloat16
LANES = 128
VMEM_LIMIT = 60 * 1024 * 1024


def group_of(n_fs, width):
    return 4 if n_fs % 4 == 0 and n_fs > 4 and width % (4 * LANES) == 0 else 1


def place(g):
    fs, core = lax.axis_index("fs"), lax.axis_index("tp")
    return lax.div(fs, g) * g, lax.rem(fs, g), core


def greet(devices):
    barrier = pltpu.get_barrier_semaphore()
    for device in devices:
        pl.semaphore_signal(barrier, inc=1, device_id=device, device_id_type=MESH)
    pl.semaphore_wait(barrier, len(devices))


def remote(src, dst, send, recv, device):
    return pltpu.make_async_remote_copy(
        src_ref=src, dst_ref=dst, send_sem=send, recv_sem=recv, device_id=device, device_id_type=MESH
    )


def at(index, size):
    return pl.ds(pl.multiple_of(index * size, size), size)


def peers(g, base, me, core):
    return [(base + lax.rem(me + k, g), core) for k in range(1, g)]


def square(base, me, core):
    x, y = lax.rem(me, 2), lax.div(me, 2)
    xn, yn = y * 2 + (1 - x), (1 - y) * 2 + x
    return xn, yn, 3 - me, (base + xn, core), (base + yn, core), (base + me, 1 - core)


class Ring:
    def __init__(self, array, rows, outer, n_out, base, me, core, g, send, recv, line):
        self.array, self.half, self.outer, self.n = array, rows // 2, outer, n_out
        self.send, self.recv, self.line, self.copies = send, recv, line, []
        self.devices = [(lax.rem(outer + d, n_out) * g + me, core) for d in (1, n_out - 1)]

    def step(self, s):
        if s:
            for c in self.copies[-2:]:
                c.wait_recv()
        if s == self.n - 1:
            return
        for way in range(2):
            owner = lax.rem(self.outer + (self.n - s if way == 0 else s), self.n)
            block = self.array.at[at(owner * 2 + way, self.half), :]
            n = s * 2 + way
            c = remote(block, block, self.send.at[self.line, n], self.recv.at[self.line, n], self.devices[way])
            c.start()
            self.copies.append(c)

    def finish(self):
        for c in self.copies:
            c.wait_send()


def ring_devices(outer, n_out, me, core, g):
    return [(lax.rem(outer + d, n_out) * g + me, core) for d in (1, n_out - 1)]


def tokens_kernel(g, n_out, cot, down, gate, up, cot_out, down_all, gate_all, up_block, send, recv, wsend, wrecv, zsend, zrecv, own):
    base, me, core = place(g)
    outer = lax.div(base, g)
    xn, yn, far, xdev, ydev, sibling = square(base, me, core)
    greet(peers(g, base, me, core) + [sibling] + ring_devices(outer, n_out, me, core, g))
    half, wide = cot.shape[0] // 2, cot.shape[1] // 2
    rows, part = down.shape[0], down.shape[1] // g
    cols = [pl.ds(0, wide), pl.ds(wide, wide)]
    mine = at(core, half)
    piece = lambda owner, i: cot_out.at[at(owner * 2 + core, half), cols[i]]
    started, passed, swaps = [], [], {}

    def go(n, a, b, device):
        c = remote(a, b, send.at[n], recv.at[n], device)
        c.start()
        started.append(c)
        return c

    def pass_on(n, owner, i):
        c = remote(piece(owner, i), piece(owner, i), send.at[n], recv.at[n], sibling)
        c.start()
        passed.append(c)

    def local_copy(i, a, b):
        c = pltpu.make_async_copy(a, b, own.at[i])
        c.start()
        return c

    def swap(i, a, b):
        swaps[i] = []
        for k in range(1, g):
            q = lax.rem(me + k, g)
            c = remote(a.at[:, at(q, part)], b, wsend.at[i, k], wrecv.at[i, k], (base + q, core))
            c.start()
            swaps[i].append(c)
        return local_copy(i, a.at[:, at(me, part)], b)

    place_of = at(outer * g + me, rows)
    own_down = swap(0, down, down_all.at[place_of, :])
    own_gate = swap(1, gate, gate_all.at[place_of, :])
    x0 = go(0, cot.at[mine, cols[0]], piece(me, 0), xdev)
    y1 = go(1, cot.at[mine, cols[1]], piece(me, 1), ydev)
    x1 = go(2, cot.at[mine, cols[1]], piece(me, 1), xdev)
    y0 = go(3, cot.at[mine, cols[0]], piece(me, 0), ydev)
    own_cot = local_copy(3, cot, cot_out.at[at(me, 2 * half), :])
    rings = []
    for i, array, mine_copy in ((0, down_all, own_down), (1, gate_all, own_gate)):
        mine_copy.wait()
        for c in swaps[i]:
            c.wait_recv()
        rings.append(Ring(array, rows * g, outer, n_out, base, me, core, g, zsend, zrecv, i))
        rings[i].step(0)
    steps = [(i, n) for n in range(1, n_out) for i in range(2)]

    def turn():
        if steps:
            i, n = steps.pop(0)
            rings[i].step(n)

    turn()
    x0.wait_recv()
    fy = go(4, piece(xn, 0), piece(xn, 0), ydev)
    pass_on(6, xn, 0)
    y1.wait_recv()
    fx = go(5, piece(yn, 1), piece(yn, 1), xdev)
    pass_on(7, yn, 1)
    own_up = swap(2, up, up_block.at[at(me, rows), :])
    turn()
    turn()
    x1.wait_recv()
    pass_on(8, xn, 1)
    y0.wait_recv()
    pass_on(9, yn, 0)
    turn()
    fy.wait_recv()
    pass_on(10, far, 0)
    fx.wait_recv()
    pass_on(11, far, 1)
    while steps:
        turn()
    own_cot.wait()
    own_up.wait()
    for c in swaps[2]:
        c.wait_recv()
    for c in started + swaps[0] + swaps[1] + swaps[2]:
        c.wait_send()
    for c in passed:
        c.wait()
    for r in rings:
        r.finish()


def middle_kernel(g, n_out, gate, up, cots, down, block, share, d_gate, d_up, up_all, gates, ups, dh, hidden, acc, send, recv, zsend, zrecv, own):
    base, me, core = place(g)
    outer = lax.div(base, g)
    greet(peers(g, base, me, core) + ring_devices(outer, n_out, me, core, g))
    first = pltpu.make_async_copy(block, up_all.at[at(outer, block.shape[0]), :], own.at[2])
    first.start()
    rows, part = gate.shape[0], gate.shape[1] // g
    copies = {}
    for k in range(1, g):
        q = lax.rem(me + k, g)
        for i, (a, b) in enumerate(((gate, gates), (up, ups))):
            c = remote(a.at[:, at(q, part)], b.at[at(me, rows), :], send.at[i, k], recv.at[i, k], (base + q, core))
            c.start()
            copies[i, k] = c
    for i, (a, b) in enumerate(((gate, gates), (up, ups))):
        c = pltpu.make_async_copy(a.at[:, at(me, part)], b.at[at(me, rows), :], own.at[i])
        c.start()
        copies[i, 0] = c
    first.wait()
    ring = Ring(up_all, block.shape[0], outer, n_out, base, me, core, g, zsend, zrecv, 0)
    ring.step(0)
    tile = rows // 2

    def multiply(i, carry):
        dh[at(i, tile), :] = jnp.dot(cots[at(i, tile), :], down[...], preferred_element_type=F32)
        return carry

    lax.fori_loop(0, 2 * g, multiply, 0)
    steps = list(range(1, n_out))
    strip = rows // 16
    for k in range(g):
        if steps:
            ring.step(steps.pop(0))
        for i in range(2):
            if k:
                copies[i, k].wait_recv()
            else:
                copies[i, k].wait()
        owner = lax.rem(me + g - k, g)

        def pointwise(i, carry):
            r = at(owner * 16 + i, strip)
            gv, uv, dv = gates[r, :].astype(F32), ups[r, :].astype(F32), dh[r, :]
            s = jax.nn.sigmoid(gv)
            gs = gv * s
            hidden[r, :] = (gs * uv).astype(BF16)
            d_gate[r, :] = (dv * uv * s * (1.0 + gv * (1.0 - s))).astype(BF16)
            d_up[r, :] = (dv * gs).astype(BF16)
            return carry

        lax.fori_loop(0, 16, pointwise, 0)
        tokens = at(owner, rows)
        piece = cots.shape[1] // 8

        def outer_product(i, carry):
            d = at(i, piece)
            new = lax.dot_general(cots[tokens, d], hidden[tokens, :], (((0,), (0,)), ((), ())), preferred_element_type=F32)
            if k:
                new = new + acc[d, :]
            if k == g - 1:
                share[d, :] = new.astype(BF16)
            else:
                acc[d, :] = new
            return carry

        lax.fori_loop(0, 8, outer_product, 0)
    while steps:
        ring.step(steps.pop(0))
    ring.finish()
    for k in range(1, g):
        for i in range(2):
            copies[i, k].wait_send()


OVER = (((1,), (1,)), ((), ()))


def input_kernel(g, d_gate, d_up, gate_w, up_w, out, give_buf, sib, mine, got, halves, send, recv):
    base, me, core = place(g)
    xn, yn, far, xdev, ydev, sibling = square(base, me, core)
    greet([xdev, ydev, sibling])
    rows, wide = out.shape[0], out.shape[1] // 2
    keep = at(core, wide)
    tile = rows // 2
    top, low = pl.ds(0, tile), pl.ds(tile, tile)
    sends, waits = [], []

    def product(side, owner, dst):
        cols = at(side, wide)

        def step(i, carry):
            r = at(owner * 2 + i, tile)
            total = lax.dot_general(d_gate[r, :], gate_w[cols, :], OVER, preferred_element_type=F32)
            total = total + lax.dot_general(d_up[r, :], up_w[cols, :], OVER, preferred_element_type=F32)
            dst[at(i, tile), :] = total.astype(BF16)
            return carry

        lax.fori_loop(0, 2, step, 0)

    def add(dst, where, src):
        dst[where, :] = (dst[where, :].astype(F32) + src[...].astype(F32)).astype(BF16)

    def go(n, a, b, device):
        c = remote(a, b, send.at[n], recv.at[n], device)
        c.start()
        sends.append(c)
        return c

    def chunk(k, owner):
        product(1 - core, owner, give_buf.at[k])
        c = go(k, give_buf.at[k], sib.at[k], sibling)
        product(core, owner, mine.at[k])
        c.wait_recv()
        add(mine.at[k], pl.ds(0, rows), sib.at[k])

    chunk(0, far)
    hx = go(4, mine.at[0, top, :], halves.at[0], xdev)
    hy = go(5, mine.at[0, low, :], halves.at[1], ydev)
    chunk(1, xn)
    waits.append(go(6, mine.at[1, top, :], got.at[0, top, :], xdev))
    chunk(2, yn)
    waits.append(go(7, mine.at[2, low, :], got.at[1, low, :], ydev))
    hy.wait_recv()
    add(mine.at[1], low, halves.at[1])
    waits.append(go(8, mine.at[1, low, :], got.at[0, low, :], xdev))
    hx.wait_recv()
    add(mine.at[2], top, halves.at[0])
    waits.append(go(9, mine.at[2, top, :], got.at[1, top, :], ydev))
    chunk(3, me)
    lasts = []
    for n, where, ready in ((10, top, (0, 3)), (11, low, (1, 2))):
        for i in ready:
            waits[i].wait_recv()
        total = mine[3, where, :].astype(F32) + got[0, where, :].astype(F32) + got[1, where, :].astype(F32)
        out[where, keep] = total.astype(BF16)
        lasts.append(go(n, out.at[where, keep], out.at[where, keep], sibling))
    for c in lasts:
        c.wait_recv()
    for c in sends:
        c.wait_send()


def down_kernel(g, down, out, got, send, recv):
    base, me, core = place(g)
    greet(peers(g, base, me, core))
    rows, wide = got.shape[1:]
    copies = []
    for k in range(1, g):
        q = lax.rem(me + k, g)
        c = remote(down.at[at(q, rows), :], got.at[k], send.at[k], recv.at[k], (base + q, core))
        c.start()
        copies.append(c)
    out[:, at(me, wide)] = down[at(me, rows), :].astype(F32)
    for k in range(1, g):
        copies[k - 1].wait_recv()
        out[:, at(lax.rem(me + g - k, g), wide)] = got[k].astype(F32)
    for c in copies:
        c.wait_send()


def call(kernel, outs, scratch, ident, cost, *args):
    vmem = pl.BlockSpec(memory_space=pltpu.VMEM)
    return pl.pallas_call(
        kernel,
        out_shape=outs,
        in_specs=[vmem] * len(args),
        out_specs=[vmem] * len(outs),
        scratch_shapes=scratch,
        compiler_params=pltpu.CompilerParams(collective_id=ident, has_side_effects=True, vmem_limit_bytes=VMEM_LIMIT),
        cost_estimate=pl.CostEstimate(flops=0, bytes_accessed=cost, transcendentals=0),
    )(*args)


def shared(g, n_fs, gate_pre, up_pre, cotangent, gate_weight, up_weight, down_weight):
    tokens, width = gate_pre.shape
    rows, depth = gate_weight.shape[0], cotangent.shape[1]
    part, n_out, all_tokens = width // g, n_fs // g, tokens * g
    sems, vmem = pltpu.SemaphoreType.DMA, pltpu.VMEM
    struct = jax.ShapeDtypeStruct
    us = 3_000_000
    columns = [[o * g + p for o in range(n_out)] for p in range(g)]
    every, block = struct((depth, part), BF16), struct((rows * g, part), BF16)
    cots, down_all, gate_w, up_block = call(
        functools.partial(tokens_kernel, g, n_out), [struct((all_tokens, depth), BF16), every, every, block],
        [sems((12,)), sems((12,)), sems((3, g)), sems((3, g)), sems((2, 2 * n_out)), sems((2, 2 * n_out)), sems((4,))],
        0, 60 * us, cotangent, down_weight, gate_weight, up_weight,
    )
    wide = struct((all_tokens, part), BF16)
    share, d_gate, d_up, up_w = call(
        functools.partial(middle_kernel, g, n_out), [every] + [wide] * 2 + [every],
        [vmem(wide.shape, BF16)] * 2
        + [vmem(wide.shape, F32), vmem(wide.shape, BF16), vmem(every.shape, F32), sems((2, g)), sems((2, g)), sems((1, 2 * n_out)), sems((1, 2 * n_out)), sems((3,))],
        1, 40 * us, gate_pre, up_pre, cots, down_all, up_block,
    )
    grad_block = lax.psum_scatter(share, "fs", scatter_dimension=0, axis_index_groups=columns, tiled=True)
    side = depth // 2
    grad_input = call(
        functools.partial(input_kernel, g), [struct((tokens, depth), BF16)],
        [vmem((4, tokens, side), BF16)] * 3 + [vmem((2, tokens, side), BF16), vmem((2, tokens // 2, side), BF16)]
        + [sems((12,)), sems((12,))],
        2, 50 * us, d_gate, d_up, gate_w, up_w,
    )[0]
    grad_down = call(
        functools.partial(down_kernel, g), [struct((rows, width), F32)],
        [vmem((g, rows, part), BF16), sems((g,)), sems((g,))], 3, 6 * us, grad_block,
    )[0]
    return grad_input, grad_down


def plain(gate_pre, up_pre, cotangent, gate_weight, up_weight, down_weight):
    gate = gate_pre.astype(F32)
    upper = up_pre.astype(F32)
    sigma = jax.nn.sigmoid(gate)
    hidden = (gate * sigma * upper).astype(BF16)
    share = lax.dot_general(cotangent, hidden, (((0,), (0,)), ((), ())), preferred_element_type=F32)
    grad_down = lax.psum_scatter(share, "fs", scatter_dimension=0, tiled=True)
    d_hidden = jnp.dot(cotangent, lax.all_gather(down_weight, "fs", axis=0, tiled=True), preferred_element_type=F32)
    d_gate = (d_hidden * upper * sigma * (1.0 + gate * (1.0 - sigma))).astype(BF16)
    d_up = (d_hidden * gate * sigma).astype(BF16)
    gate_w, up_w = lax.all_gather((gate_weight, up_weight), "fs", axis=0, tiled=True)
    over = (((1,), (1,)), ((), ()))
    partial_sum = lax.dot_general(d_gate, gate_w, over, preferred_element_type=F32)
    partial_sum = partial_sum + lax.dot_general(d_up, up_w, over, preferred_element_type=F32)
    grad_input = lax.psum(partial_sum.astype(BF16), "tp").astype(F32).astype(BF16)
    return grad_input, grad_down


def solution(mesh):
    n_fs, n_tp = mesh.shape["fs"], mesh.shape["tp"]

    def local(*args):
        g = group_of(n_fs, args[0].shape[1]) if n_tp == 2 else 1
        return shared(g, n_fs, *args) if g > 1 else plain(*args)

    both, rows = P("fs", "tp"), P("fs", None)
    return jax.shard_map(
        local, mesh=mesh, in_specs=(both, both, rows, both, both, both), out_specs=(rows, both), check_vma=False
    )
```
